32 devices in a mesh: grp: 2 (over y), st: 4 (over z), tp: 4 (over x, core).
Axes of the slice: x: 2, y: 2, z: 4, core: 2. Of those that a mesh axis runs over, the one named last changes fastest.
Arguments:
- pass_ids: int32 [64, 4], P(('grp', 'st')), parts along dimension 0, may hold values from 0 to 63, as said below
- store: bfloat16 [64, 64, 2048], P('st', None, 'tp'), may hold values from -6 to 6
- queries: bfloat16 [8192, 1024], P(('grp', 'st'), 'tp'), parts along dimension 0, may hold values from -40 to 40
- gate_pre: bfloat16 [8192, 1024], P(('grp', 'st'), 'tp'), parts along dimension 0, may hold values from -6 to 6
- w_query: bfloat16 [2048, 1024], P(None, 'tp'), may hold values from -0.125 to 0.125
- w_gate: bfloat16 [2048, 1024], P(None, 'tp'), may hold values from -0.125 to 0.125
- w_key: bfloat16 [2048, 1024], P(None, 'tp'), may hold values from -0.125 to 0.125
- w_value: bfloat16 [2048, 1024], P(None, 'tp'), may hold values from -0.125 to 0.125
- d_mem: bfloat16 [8192, 1024], P(('grp', 'st'), 'tp'), parts along dimension 0, may hold values from -6 to 6
Outputs:
- d_tokens: bfloat16 [8192, 2048], P(('grp', 'st', 'tp')), parts along dimension 0
- d_store: bfloat16 [128, 64, 2048], P(('grp', 'st', 'tp')), parts along dimension 0
- d_wkey: float32 [4096, 1024], P(('grp', 'st'), 'tp'), parts along dimension 0
The draws below stay inside these ranges and needn't reach their ends.
There are 2 independent parts, one for each index of `grp`. The reference program is written for one: setup_inputs(seed, part) draws one part's arguments, and reference() takes and returns one part's arrays. A program takes and returns all parts, laid end to end along the dimension named above; an argument that names none is the same for every part. Nothing has to cross between parts.
Inputs may be any that keep to these rules, and one draw needn't show every extreme that they name: `pass_ids`: the 8 blocks of one index of st name at most 8 passages (counted with repetition) held by any one index of st o, that is passages o * 16 to o * 16 + 15. Every index of st takes exactly 8 passages from each of 4 indices of st and none from the others, so the bound 8 is reached by every index.
All inputs are finite; a program needn't handle non-finite values.
Results may differ from the reference program's by a relative error of at most 0.02.
Values may be sent and summed in bfloat16 or wider, within the bound.
No kernel may reach another device: no remote copies, remote signals or barrier semaphores. Data moves between devices by JAX's collectives and lax.ppermute only.
A program may use at most 128 MiB of HBM per device.

```python
import jax
import jax.numpy as jnp
from jax import lax

D = 2048
HD = 256
MH = 4
BLK = 128
PB = 4
PL = 64
PASS_DEV = 16
MW = 1024
NBLK_DEV = 8
NBLK = 32
TOKENS = 4096
NPASS = 64
MOST = 8
N_ST = 4
N_TP = 4


def draw_pass_ids(key, part):
    folded = jax.random.fold_in(key, 17)
    key_hot, key_rank, key_order, key_pick, key_shift = jax.random.split(folded, 5)
    total_req = NBLK_DEV * PB
    used_owners = total_req // MOST
    device = jnp.arange(N_ST, dtype=jnp.int32)[:, None]
    owner_row = jnp.arange(N_ST, dtype=jnp.int32)[None, :]
    hottest = jax.random.randint(key_hot, (), 0, N_ST)
    levels = jnp.where(owner_row == hottest, 3, jnp.where(owner_row == (device - 1) % N_ST, 2, jnp.where(owner_row == (device + N_ST // 2) % N_ST, 1, 0)))
    jitter = jax.random.randint(key_rank, (N_ST, N_ST), 0, 1000)
    scores = levels * (1000 * N_ST) + jitter * N_ST + owner_row
    chosen = lax.top_k(scores, used_owners)[1].astype(jnp.int32)
    owners = jnp.repeat(chosen, MOST, axis=1)
    order_keys = jax.random.randint(key_order, (N_ST, total_req), 0, 1000) * total_req + jnp.arange(total_req, dtype=jnp.int32)[None, :]
    ordering = jnp.argsort(order_keys, axis=1)
    owners = jnp.take_along_axis(owners, ordering, axis=1)
    samples = jax.random.randint(key_pick, (3, N_ST, total_req), 0, PASS_DEV)
    popular = jnp.min(samples, axis=0)
    offsets = jax.random.randint(key_shift, (N_ST,), 0, PASS_DEV)
    within = (popular + offsets[owners]) % PASS_DEV
    passage_ids = owners * PASS_DEV + within
    return passage_ids.reshape(N_ST * NBLK_DEV, PB).astype(jnp.int32)


def draw_queries(key, part):
    folded = jax.random.fold_in(key, 23)
    key_base = jax.random.fold_in(folded, 0)
    base = jnp.clip(jax.random.normal(key_base, (TOKENS, MW), jnp.float32), -6.0, 6.0)
    return base.astype(jnp.bfloat16)


def level_of(own_key, dims, cuts, least, high):
    def one(dim, shards_of):
        steps = jax.random.uniform(jax.random.fold_in(jax.random.fold_in(own_key, 6), dim), (shards_of,), jnp.float32, least / len(cuts), high / len(cuts))
        return jnp.repeat(jnp.exp(steps), dims[dim] // shards_of).reshape((-1,) + (1,) * (len(dims) - dim - 1))

    loudness = one(*cuts[0])
    for cut in cuts[1:]:
        loudness = loudness * one(*cut)
    return loudness


def bell_draw(key, shape, deviation, reach, cuts=(), kind=jnp.bfloat16):
    array = jax.random.normal(key, shape, jnp.float32) * deviation
    if len(cuts) > 0:
        array = level_of(key, shape, cuts, -0.22, 0.18) * array
    return jnp.clip(array, min=-reach, max=reach).astype(kind)


def setup_inputs(seed: int = 0, part: int = 0) -> dict:
    keys = jax.random.split(jax.random.key(seed), 10)
    part_keys = jax.random.split(jax.random.fold_in(keys[9], part), 10)
    return {
        "pass_ids": draw_pass_ids(jax.random.fold_in(jax.random.fold_in(keys[9], part), 71), part),
        "store": bell_draw(keys[1], (NPASS, PL, D), 1.0, 6.0, ((0, 4), (2, 4))),
        "queries": draw_queries(jax.random.fold_in(jax.random.fold_in(keys[9], part), 71), part),
        "gate_pre": bell_draw(part_keys[3], (TOKENS, MW), 1.5, 6.0, ((0, 4), (1, 4))),
        "w_query": bell_draw(keys[4], (D, MW), D ** -0.5, 0.125, ((1, 4),)),
        "w_gate": bell_draw(keys[5], (D, MW), D ** -0.5, 0.125, ((1, 4),)),
        "w_key": bell_draw(keys[6], (D, MW), D ** -0.5, 0.125, ((1, 4),)),
        "w_value": bell_draw(keys[7], (D, MW), D ** -0.5, 0.125, ((1, 4),)),
        "d_mem": bell_draw(part_keys[8], (TOKENS, MW), 1.0, 6.0, ((0, 4), (1, 4))),
    }


def rounded_copy(values):
    return lax.optimization_barrier(values.astype(jnp.bfloat16)).astype(jnp.float32)


def reference(pass_ids, store, queries, gate_pre, w_query, w_gate, w_key, w_value, d_mem):
    flat_rows = store.reshape(NPASS * PL, D)
    keys_all = jnp.dot(flat_rows, w_key, preferred_element_type=jnp.float32).astype(jnp.bfloat16).reshape(NPASS, PL, MW)
    values_all = jnp.dot(flat_rows, w_value, preferred_element_type=jnp.float32).astype(jnp.bfloat16).reshape(NPASS, PL, MW)
    request_ids = pass_ids.reshape(-1).astype(jnp.int32)
    key_rows = keys_all[request_ids].reshape(NBLK, PB * PL, MH, HD).astype(jnp.float32)
    value_rows = values_all[request_ids].reshape(NBLK, PB * PL, MH, HD).astype(jnp.float32)
    query_rows = queries.reshape(NBLK, BLK, MH, HD).astype(jnp.float32)
    score_scale = HD ** -0.5
    scores = jnp.einsum('nqhd,nkhd->nhqk', query_rows, key_rows) * score_scale
    shifted = jnp.exp(scores - jnp.max(scores, axis=-1, keepdims=True))
    prob_rows = shifted / jnp.sum(shifted, axis=-1, keepdims=True)
    probs_low = rounded_copy(prob_rows)
    attended = jnp.einsum('nhqk,nkhd->nqhd', probs_low, value_rows).reshape(TOKENS, MW)
    gate_vals = gate_pre.astype(jnp.float32)
    sigmoid_vals = jax.nn.sigmoid(gate_vals)
    mem_grad = d_mem.astype(jnp.float32)
    attended_grad = rounded_copy(gate_vals * sigmoid_vals * mem_grad)
    gate_grad = rounded_copy(mem_grad * attended * sigmoid_vals * (1.0 + gate_vals * (1.0 - sigmoid_vals)))
    attended_four = attended_grad.reshape(NBLK, BLK, MH, HD)
    prob_grad = jnp.einsum('nqhd,nkhd->nhqk', attended_four, value_rows)
    score_grad = rounded_copy(score_scale * prob_rows * (prob_grad - jnp.sum(prob_rows * prob_grad, axis=-1, keepdims=True)))
    query_grad = rounded_copy(jnp.einsum('nhqk,nkhd->nqhd', score_grad, key_rows).reshape(TOKENS, MW))
    key_grad = rounded_copy(jnp.einsum('nhqk,nqhd->nkhd', score_grad, query_rows)).reshape(NBLK * PB, PL, MW)
    value_grad = rounded_copy(jnp.einsum('nhqk,nqhd->nkhd', probs_low, attended_four)).reshape(NBLK * PB, PL, MW)
    key_sums = jax.ops.segment_sum(key_grad, request_ids, NPASS).astype(jnp.bfloat16).reshape(NPASS * PL, MW)
    value_sums = jax.ops.segment_sum(value_grad, request_ids, NPASS).astype(jnp.bfloat16).reshape(NPASS * PL, MW)
    d_wkey = jnp.dot(flat_rows.T, key_sums, preferred_element_type=jnp.float32)
    group_width = MW // N_TP
    query_low = query_grad.astype(jnp.bfloat16)
    gate_low = gate_grad.astype(jnp.bfloat16)
    store_total = jnp.zeros((NPASS * PL, D), jnp.float32)
    token_total = jnp.zeros((TOKENS, D), jnp.float32)
    for group_index in range(N_TP):
        col_low = group_index * group_width
        col_high = col_low + group_width
        store_part = jnp.dot(key_sums[:, col_low:col_high], w_key[:, col_low:col_high].T, preferred_element_type=jnp.float32)
        store_part = store_part + jnp.dot(value_sums[:, col_low:col_high], w_value[:, col_low:col_high].T, preferred_element_type=jnp.float32)
        store_total = store_total + rounded_copy(store_part)
        token_part = jnp.dot(query_low[:, col_low:col_high], w_query[:, col_low:col_high].T, preferred_element_type=jnp.float32)
        token_part = token_part + jnp.dot(gate_low[:, col_low:col_high], w_gate[:, col_low:col_high].T, preferred_element_type=jnp.float32)
        token_total = token_total + rounded_copy(token_part)
    d_store = store_total.astype(jnp.bfloat16).reshape(NPASS, PL, D)
    d_tokens = token_total.astype(jnp.bfloat16)
    return (d_tokens, d_store, d_wkey)
```

```python
import functools

import jax
import jax.numpy as jnp
from jax import lax
from jax.experimental import pallas as pl
from jax.experimental.pallas import tpu as pltpu
from jax.sharding import PartitionSpec as P

HD = 256
BLK = 128
PB = 4
F32 = jnp.float32
BF16 = jnp.bfloat16
NT = (((1,), (1,)), ((), ()))
TN = (((0,), (0,)), ((), ()))
NN = (((1,), (0,)), ((), ()))


def mm(a, b, dims):
    return lax.dot_general(a, b, dims, preferred_element_type=F32)


def whole(shape):
    return pl.BlockSpec(shape, lambda *_: (0,) * len(shape))


def params(*semantics):
    return pltpu.CompilerParams(dimension_semantics=semantics, vmem_limit_bytes=48 << 20)


def cost(flops, moved):
    return pl.CostEstimate(flops=flops, transcendentals=0, bytes_accessed=moved)


def table_body(ring, passages, depth, requests, meta, *refs):
    count = refs[0].shape[0] if not ring else len(refs) - 3
    ids = refs[:-3]
    asked, place, seen = refs[-3:]
    me = meta[0]

    def id_of(k, r):
        return ids[k][r] if ring else ids[0][k, r]

    for k in range(count):
        for i in range(depth):
            asked[k * depth + i] = -1

        def step(r, found, k=k):
            local = id_of(k, r) - me * passages
            hit = (local >= 0) & (local < passages)

            @pl.when(hit)
            def _():
                asked[k * depth + found] = local

            return found + hit.astype(jnp.int32)

        lax.fori_loop(0, requests, step, jnp.int32(0))
        seen[k] = 0

    def own(r, carry):
        wanted = id_of(0, r) if ring else ids[0][me, r]
        owner = lax.div(wanted, passages)
        rank = seen[owner]
        seen[owner] = rank + 1
        group = lax.rem(me - owner + count, count) if ring else owner
        place[r] = group * depth + rank
        return carry

    lax.fori_loop(0, requests, own, jnp.int32(0))


def tables(ring, meta, ids, count, passages, depth, requests):
    smem = pl.BlockSpec(memory_space=pltpu.SMEM)
    return pl.pallas_call(
        functools.partial(table_body, ring, passages, depth, requests),
        in_specs=[smem] * (1 + len(ids)),
        out_specs=[smem, smem],
        out_shape=[
            jax.ShapeDtypeStruct((count * depth,), jnp.int32),
            jax.ShapeDtypeStruct((requests,), jnp.int32),
        ],
        scratch_shapes=[pltpu.SMEM((count,), jnp.int32)],
        name="tables",
    )(meta, *ids)


def project_body(shards, steps, slots, pass_len, meta, asked, *refs):
    rows_in = refs[:shards]
    weight = refs[shards]
    outs = refs[shards + 1 : -1]
    held = refs[-1]
    step = pl.program_id(0)
    chunk, width = rows_in[0].shape
    total = None
    for i in range(shards):
        begin = pl.multiple_of(jnp.bitwise_xor(meta[1], i) * width, width)
        term = mm(rows_in[i][...], weight[pl.ds(begin, width), :], NN)
        total = term if total is None else total + term
    held[pl.ds(pl.multiple_of(step * chunk, chunk), chunk), :] = total.astype(BF16)

    @pl.when(step == steps - 1)
    def _():
        per = slots // len(outs)
        for slot in range(slots):
            passage = jnp.maximum(asked[slot], 0)
            begin = pl.multiple_of(passage * pass_len, pass_len)
            at = (slot % per) * pass_len
            outs[slot // per][at : at + pass_len, :] = held[pl.ds(begin, pass_len), :]


def project(meta, asked, pieces, weight, pass_len, parts, name):
    rows, width = pieces[0].shape
    cols = weight.shape[1]
    steps = 4
    slots = asked.shape[0]
    part_rows = slots * pass_len // parts
    grid_spec = pltpu.PrefetchScalarGridSpec(
        num_scalar_prefetch=2,
        grid=(steps,),
        in_specs=[pl.BlockSpec((rows // steps, width), lambda i, *_: (i, 0))] * len(pieces)
        + [whole(weight.shape)],
        out_specs=[whole((part_rows, cols))] * parts,
        scratch_shapes=[pltpu.VMEM((rows, cols), BF16)],
    )
    return pl.pallas_call(
        functools.partial(project_body, len(pieces), steps, slots, pass_len),
        grid_spec=grid_spec,
        out_shape=[jax.ShapeDtypeStruct((part_rows, cols), BF16)] * parts,
        compiler_params=params("arbitrary"),
        cost_estimate=cost(2 * rows * weight.shape[0] * cols, 2 * rows * weight.shape[0]),
        name=name,
    )(meta, asked, *pieces, weight)


def join(parts, held):
    at = 0
    for part in parts:
        held[at : at + part.shape[0], :] = part[...]
        at += part.shape[0]


def split(held, parts):
    at = 0
    for part in parts:
        part[...] = held[at : at + part.shape[0], :]
        at += part.shape[0]


def block_rows(held, place, block, pass_len):
    tiles = []
    for j in range(PB):
        begin = pl.multiple_of(place[block * PB + j] * pass_len, pass_len)
        tiles.append(held[pl.ds(begin, pass_len), :])
    return jnp.concatenate(tiles, axis=0)


def put_rows(held, place, block, pass_len, values):
    for j in range(PB):
        begin = pl.multiple_of(place[block * PB + j] * pass_len, pass_len)
        held[pl.ds(begin, pass_len), :] = values[j * pass_len : (j + 1) * pass_len, :]


def first_body(parts, pass_len, spare, place, *refs):
    keys = refs[:parts]
    queries, gate, mem = refs[parts : parts + 3]
    value_out = refs[parts + 3 : 2 * parts + 3]
    probs, mixed = refs[2 * parts + 3 : 2 * parts + 5]
    held, grads = refs[2 * parts + 5 :]
    block = pl.program_id(0)

    @pl.when(block == 0)
    def _():
        join(keys, held)
        if spare:
            grads[...] = jnp.zeros_like(grads)

    rows = block_rows(held, place, block, pass_len)
    scores = mm(rows, queries[...], NT) * (HD**-0.5)
    shifted = jnp.exp(scores - jnp.max(scores, axis=0, keepdims=True))
    prob = shifted / jnp.sum(shifted, axis=0, keepdims=True)
    probs[...] = prob
    g = gate[...].astype(F32)
    low = (g * jax.nn.sigmoid(g) * mem[...].astype(F32)).astype(BF16)
    mixed[...] = low
    put_rows(grads, place, block, pass_len, mm(prob.astype(BF16), low, NN).astype(BF16))

    @pl.when(block == pl.num_programs(0) - 1)
    def _():
        split(grads, value_out)


def first(place, keys, queries, gate, mem, pass_len):
    parts = len(keys)
    tok, cols = queries.shape
    blocks = tok // BLK
    slot_rows = sum(k.shape[0] for k in keys)
    tok_spec = pl.BlockSpec((BLK, cols), lambda i, *_: (i, 0))
    keyed = PB * pass_len
    grid_spec = pltpu.PrefetchScalarGridSpec(
        num_scalar_prefetch=1,
        grid=(blocks,),
        in_specs=[whole(k.shape) for k in keys] + [tok_spec] * 3,
        out_specs=[whole(k.shape) for k in keys]
        + [pl.BlockSpec((keyed, BLK), lambda i, *_: (i, 0)), tok_spec],
        scratch_shapes=[pltpu.VMEM((slot_rows, cols), BF16)] * 2,
    )
    out = pl.pallas_call(
        functools.partial(first_body, parts, pass_len, slot_rows > blocks * keyed),
        grid_spec=grid_spec,
        out_shape=[jax.ShapeDtypeStruct(k.shape, BF16) for k in keys]
        + [
            jax.ShapeDtypeStruct((blocks * keyed, BLK), F32),
            jax.ShapeDtypeStruct((tok, cols), BF16),
        ],
        compiler_params=params("arbitrary"),
        cost_estimate=cost(4 * tok * keyed * cols, 8 * tok * cols),
        name="first",
    )(place, *keys, queries, gate, mem)
    return out[:parts], out[parts], out[parts + 1]


def second_body(parts, pass_len, spare, place, *refs):
    values = refs[:parts]
    queries, probs, mixed = refs[parts : parts + 3]
    key_out = refs[parts + 3 : 2 * parts + 3]
    score_out = refs[2 * parts + 3]
    held, grads = refs[2 * parts + 4 :]
    block = pl.program_id(0)

    @pl.when(block == 0)
    def _():
        join(values, held)
        if spare:
            grads[...] = jnp.zeros_like(grads)

    rows = block_rows(held, place, block, pass_len)
    prob = probs[...]
    prob_grad = mm(rows, mixed[...], NT)
    inner = jnp.sum(prob * prob_grad, axis=0, keepdims=True)
    score_grad = ((HD**-0.5) * prob * (prob_grad - inner)).astype(BF16)
    score_out[...] = score_grad
    put_rows(grads, place, block, pass_len, mm(score_grad, queries[...], NN).astype(BF16))

    @pl.when(block == pl.num_programs(0) - 1)
    def _():
        split(grads, key_out)


def second(place, values, queries, probs, mixed, pass_len):
    parts = len(values)
    tok, cols = queries.shape
    blocks = tok // BLK
    slot_rows = sum(v.shape[0] for v in values)
    tok_spec = pl.BlockSpec((BLK, cols), lambda i, *_: (i, 0))
    keyed = PB * pass_len
    pair_spec = pl.BlockSpec((keyed, BLK), lambda i, *_: (i, 0))
    grid_spec = pltpu.PrefetchScalarGridSpec(
        num_scalar_prefetch=1,
        grid=(blocks,),
        in_specs=[whole(v.shape) for v in values] + [tok_spec, pair_spec, tok_spec],
        out_specs=[whole(v.shape) for v in values] + [pair_spec],
        scratch_shapes=[pltpu.VMEM((slot_rows, cols), BF16)] * 2,
    )
    out = pl.pallas_call(
        functools.partial(second_body, parts, pass_len, slot_rows > blocks * keyed),
        grid_spec=grid_spec,
        out_shape=[jax.ShapeDtypeStruct(v.shape, BF16) for v in values]
        + [jax.ShapeDtypeStruct((blocks * keyed, BLK), BF16)],
        compiler_params=params("arbitrary"),
        cost_estimate=cost(4 * tok * keyed * cols, 8 * tok * cols),
        name="second",
    )(place, *values, queries, probs, mixed)
    return out[:parts], out[parts]


def third_body(parts, pass_len, place, *refs):
    keys = refs[:parts]
    values = refs[parts : 2 * parts]
    probs, score_grad, gate, mem, query_out, gate_out, held_k, held_v = refs[2 * parts :]
    block = pl.program_id(0)

    @pl.when(block == 0)
    def _():
        join(keys, held_k)
        join(values, held_v)

    key_rows = block_rows(held_k, place, block, pass_len)
    value_rows = block_rows(held_v, place, block, pass_len)
    query_out[...] = mm(score_grad[...], key_rows, TN).astype(BF16)
    attended = mm(probs[...].astype(BF16), value_rows, TN)
    g = gate[...].astype(F32)
    sig = jax.nn.sigmoid(g)
    gate_out[...] = (mem[...].astype(F32) * attended * sig * (1.0 + g * (1.0 - sig))).astype(BF16)


def third(place, keys, values, probs, score_grad, gate, mem, pass_len):
    parts = len(keys)
    tok, cols = gate.shape
    blocks = tok // BLK
    slot_rows = sum(k.shape[0] for k in keys)
    tok_spec = pl.BlockSpec((BLK, cols), lambda i, *_: (i, 0))
    keyed = PB * pass_len
    pair_spec = pl.BlockSpec((keyed, BLK), lambda i, *_: (i, 0))
    grid_spec = pltpu.PrefetchScalarGridSpec(
        num_scalar_prefetch=1,
        grid=(blocks,),
        in_specs=[whole(k.shape) for k in keys] * 2 + [pair_spec, pair_spec, tok_spec, tok_spec],
        out_specs=[tok_spec, tok_spec],
        scratch_shapes=[pltpu.VMEM((slot_rows, cols), BF16)] * 2,
    )
    return pl.pallas_call(
        functools.partial(third_body, parts, pass_len),
        grid_spec=grid_spec,
        out_shape=[jax.ShapeDtypeStruct((tok, cols), BF16)] * 2,
        compiler_params=params("arbitrary"),
        cost_estimate=cost(4 * tok * keyed * cols, 12 * tok * cols),
        name="third",
    )(place, *keys, *values, probs, score_grad, gate, mem)


def sum_slots(parts, asked, pass_len, total):
    total[...] = jnp.zeros_like(total)
    slots = asked.shape[0]
    per = slots // len(parts)
    for slot in range(slots):
        passage = asked[slot]

        @pl.when(passage >= 0)
        def _(slot=slot, passage=passage):
            at = pl.ds(pl.multiple_of(passage * pass_len, pass_len), pass_len)
            begin = (slot % per) * pass_len
            total[at, :] += parts[slot // per][begin : begin + pass_len, :].astype(F32)


def sums_body(parts, pass_len, asked, *refs):
    out, total = refs[parts:]
    sum_slots(refs[:parts], asked, pass_len, total)
    out[...] = total[...].astype(BF16)


def passage_sums(asked, grads, rows, pass_len, name):
    cols = grads[0].shape[1]
    grid_spec = pltpu.PrefetchScalarGridSpec(
        num_scalar_prefetch=1,
        grid=(1,),
        in_specs=[whole(g.shape) for g in grads],
        out_specs=whole((rows, cols)),
        scratch_shapes=[pltpu.VMEM((rows, cols), F32)],
    )
    return pl.pallas_call(
        functools.partial(sums_body, len(grads), pass_len),
        grid_spec=grid_spec,
        out_shape=jax.ShapeDtypeStruct((rows, cols), BF16),
        compiler_params=params("arbitrary"),
        cost_estimate=cost(10**7, 8 * rows * cols),
        name=name,
    )(asked, *grads)


def weight_body(shards, ring, meta, *refs):
    pieces = refs[:shards]
    sums = refs[shards]
    outs = refs[shards + 1 : -1]
    held = refs[-1]
    turned = sums[...].astype(F32).T.astype(BF16)
    width = pieces[0].shape[1]
    for i in range(shards):
        begin = pl.multiple_of(jnp.bitwise_xor(meta[1], i) * width, width)
        held[:, pl.ds(begin, width)] = mm(turned, pieces[i][...], NN)
    if not ring:
        outs[0][...] = held[...].T
        return
    count = len(outs)
    for k in range(count):
        share = outs[k].shape[1]
        begin = pl.multiple_of(lax.rem(meta[0] + k, count) * share, share)
        outs[k][...] = held[:, pl.ds(begin, share)].astype(outs[k].dtype)


def weight_grad(meta, pieces, sums, ring, count):
    rows, width = pieces[0].shape
    cols = sums.shape[1]
    full = width * len(pieces)
    if ring:
        shapes = [
            jax.ShapeDtypeStruct((cols, full // count), F32 if k == 0 else BF16)
            for k in range(count)
        ]
    else:
        shapes = [jax.ShapeDtypeStruct((full, cols), F32)]
    grid_spec = pltpu.PrefetchScalarGridSpec(
        num_scalar_prefetch=1,
        grid=(1,),
        in_specs=[whole(p.shape) for p in pieces] + [whole(sums.shape)],
        out_specs=[whole(s.shape) for s in shapes],
        scratch_shapes=[pltpu.VMEM((cols, full), F32)],
    )
    return pl.pallas_call(
        functools.partial(weight_body, len(pieces), ring),
        grid_spec=grid_spec,
        out_shape=shapes,
        compiler_params=params("arbitrary"),
        cost_estimate=cost(2 * rows * full * cols, 2 * rows * full),
        name="weight_grad",
    )(meta, *pieces, sums)


def turn_body(*refs):
    total = refs[0][...]
    for part in refs[1:-1]:
        total = total + part[...].astype(F32)
    refs[-1][...] = total.T


def turn_sum(parts):
    cols, share = parts[0].shape
    return pl.pallas_call(
        turn_body,
        out_shape=jax.ShapeDtypeStruct((share, cols), F32),
        compiler_params=pltpu.CompilerParams(vmem_limit_bytes=48 << 20),
        cost_estimate=cost(10**6, 10 * cols * share),
        name="turn_sum",
    )(*parts)


def rows_body(terms, meta, *refs):
    out = refs[2 * terms]
    total = mm(refs[0][...], refs[terms][...], NT)
    for i in range(1, terms):
        total = total + mm(refs[i][...], refs[terms + i][...], NT)
    out[...] = total.astype(out.dtype)


def row_term(meta, flip, grads, weights, quarters, dtype, name):
    rows, cols = grads[0].shape
    model = weights[0].shape[0]
    steps = 4
    terms = len(grads)
    grid_spec = pltpu.PrefetchScalarGridSpec(
        num_scalar_prefetch=1,
        grid=(steps,),
        in_specs=[
            pl.BlockSpec((rows // quarters, cols), lambda i, m: (jnp.bitwise_xor(m[1], flip), 0))
        ]
        * terms
        + [pl.BlockSpec((model // steps, cols), lambda i, m: (i, 0))] * terms,
        out_specs=pl.BlockSpec((rows // quarters, model // steps), lambda i, m: (0, i)),
    )
    return pl.pallas_call(
        functools.partial(rows_body, terms),
        grid_spec=grid_spec,
        out_shape=jax.ShapeDtypeStruct((rows // quarters, model), dtype),
        compiler_params=params("arbitrary"),
        cost_estimate=cost(
            2 * terms * rows // quarters * cols * model, 2 * terms * cols * model
        ),
        name=name,
    )(meta, *grads, *weights)


def local(pass_ids, store, queries, gate_pre, w_query, w_gate, w_key, w_value, d_mem):
    st_count = lax.axis_size("st")
    tp_count = lax.axis_size("tp")
    if tp_count != 4:
        raise ValueError("tp")
    passages, pass_len, width = store.shape
    blocks = queries.shape[0] // BLK
    requests = blocks * PB
    depth = max(2, requests // st_count)
    ring = st_count <= 8
    parts = st_count if ring else 1
    meta = jnp.stack([lax.axis_index("st"), lax.axis_index("tp")]).astype(jnp.int32)

    def flip(value, bit):
        return lax.ppermute(value, "tp", [(i, i ^ bit) for i in range(tp_count)])

    def shift(value, k):
        return lax.ppermute(value, "st", [(i, (i + k) % st_count) for i in range(st_count)])

    def exchange(values, sign):
        if ring:
            return [values[0]] + [shift(values[k], sign * k) for k in range(1, st_count)]
        return [lax.all_to_all(values[0], "st", split_axis=0, concat_axis=0, tiled=True)]

    flat = store.reshape(passages * pass_len, width)
    across = flip(flat, 2)
    pieces = [flat, flip(flat, 1), across, flip(across, 1)]

    own_ids = pass_ids.reshape(requests)
    if ring:
        ids = [own_ids] + [shift(own_ids, -k) for k in range(1, st_count)]
    else:
        ids = [lax.all_gather(own_ids, "st", axis=0, tiled=False)]
    asked, place = tables(ring, meta, ids, st_count, passages, depth, requests)

    keys_out = project(meta, asked, pieces, w_key, pass_len, parts, "project_keys")
    keys_in = exchange(keys_out, 1)
    values_out = project(meta, asked, pieces, w_value, pass_len, parts, "project_values")
    values_in = exchange(values_out, 1)

    value_grads, probs, mixed = first(place, keys_in, queries, gate_pre, d_mem, pass_len)
    value_back = exchange(value_grads, -1)
    key_grads, score_grad = second(place, values_in, queries, probs, mixed, pass_len)
    key_back = exchange(key_grads, -1)
    query_grad, gate_grad = third(
        place, keys_in, values_in, probs, score_grad, gate_pre, d_mem, pass_len
    )

    rows = passages * pass_len
    weights_t = [w_query, w_gate, flip(w_query, 1), flip(w_gate, 1)]
    grads_t = [query_grad, gate_grad, flip(query_grad, 1), flip(gate_grad, 1)]
    sent_t = flip(row_term(meta, 2, grads_t, weights_t, tp_count, BF16, "tokens_send"), 2)
    kept_t = row_term(meta, 0, grads_t, weights_t, tp_count, F32, "tokens_keep")
    d_tokens = (kept_t + sent_t.astype(F32)).astype(BF16)

    value_sums = passage_sums(asked, value_back, rows, pass_len, "value_sums")
    key_sums = passage_sums(asked, key_back, rows, pass_len, "key_sums")
    weight_parts = weight_grad(meta, pieces, key_sums, ring, st_count)
    if ring:
        d_wkey = turn_sum(exchange(weight_parts, 1))
    else:
        d_wkey = lax.psum_scatter(weight_parts[0], "st", scatter_dimension=0, tiled=True)

    weights_s = [w_key, w_value, flip(w_key, 1), flip(w_value, 1)]
    grads_s = [key_sums, value_sums, flip(key_sums, 1), flip(value_sums, 1)]
    sent_s = flip(row_term(meta, 2, grads_s, weights_s, tp_count, BF16, "store_send"), 2)
    kept_s = row_term(meta, 0, grads_s, weights_s, tp_count, F32, "store_keep")
    d_store = (kept_s + sent_s.astype(F32)).astype(BF16)
    d_store = d_store.reshape(passages // tp_count, pass_len, d_store.shape[1])
    return (d_tokens, d_store, d_wkey)


def solution(mesh):
    return jax.shard_map(
        local,
        mesh=mesh,
        in_specs=(
            P(("grp", "st"), None),
            P("st", None, "tp"),
            P(("grp", "st"), "tp"),
            P(("grp", "st"), "tp"),
            P(None, "tp"),
            P(None, "tp"),
            P(None, "tp"),
            P(None, "tp"),
            P(("grp", "st"), "tp"),
        ),
        out_specs=(
            P(("grp", "st", "tp"), None),
            P(("grp", "st", "tp"), None, None),
            P(("grp", "st"), "tp"),
        ),
        check_vma=False,
    )
```
